32 devices in a mesh: ep: 8 (over z, y), tp: 4 (over x, core).
Axes of the slice: x: 2, y: 2, z: 4, core: 2. Of those that a mesh axis runs over, the one named last changes fastest.
Arguments:
- hidden: bfloat16 [512, 2048], P('ep'), may hold values from -10 to 10
- mix_gain: bfloat16 [2048], replicated, may hold values from 0.099609375 to 1.8984375
- proj_x: bfloat16 [2048, 2048], P('ep', 'tp'), may hold values from -0.125 to 0.125
- proj_y: bfloat16 [2048, 2048], P('ep', 'tp'), may hold values from -0.125 to 0.125
- conv_taps: bfloat16 [4, 2048], P(None, 'tp'), may hold values from -3 to 3
- input_gate: bfloat16 [32, 64, 64], P('tp'), may hold values from -0.75 to 0.75
- decay_gate: bfloat16 [32, 64, 64], P('tp'), may hold values from -0.75 to 0.75
- decay_param: float32 [2048], P('tp'), may hold values from 1 to 6
- proj_out: bfloat16 [2048, 2048], P('tp'), may hold values from -0.125 to 0.125
- conv_state: bfloat16 [512, 3, 2048], P('ep', None, 'tp'), may hold values from -6 to 6
- lru_state: float32 [512, 2048], P('ep', 'tp'), may hold values from -6 to 6
- ffn_gain: bfloat16 [2048], replicated, may hold values from 0.099609375 to 1.8984375
- routes: int32 [512, 2], P('ep'), may hold values from 0 to 7, all different within a row; in each aligned block of 64 rows (0 to 63, 64 to 127, ...) at most 18 rows name the same one
- route_weights: float32 [512, 2], P('ep'), may hold values from 0.2 to 1
- expert_gate: bfloat16 [8, 2048, 3072], P('ep', None, 'tp'), may hold values from -0.125 to 0.125
- expert_up: bfloat16 [8, 2048, 3072], P('ep', None, 'tp'), may hold values from -0.125 to 0.125
- expert_down: bfloat16 [8, 3072, 2048], P('ep', 'tp'), may hold values from -0.109375 to 0.109375
- dense_gate: bfloat16 [2048, 6144], P('tp', 'ep'), may hold values from -0.125 to 0.125
- dense_up: bfloat16 [2048, 6144], P('tp', 'ep'), may hold values from -0.125 to 0.125
- dense_down: bfloat16 [6144, 2048], P('ep', 'tp'), may hold values from -0.078125 to 0.078125
- branch_gate: float32 [2048], P('tp'), may hold values from -4 to 4
Outputs:
- new_hidden: bfloat16 [512, 2048], P('ep', 'tp')
- new_lru: float32 [512, 2048], P('ep', 'tp')
- new_conv: bfloat16 [512, 3, 2048], P('ep', None, 'tp')
The draws below stay inside these ranges and needn't reach their ends.
Inputs may be any that keep to these rules, and one draw needn't show every extreme that they name: `routes`: each row names 2 different experts. In the 64 rows of one index of ep, no expert is named by more than 18 rows, a bound that some block reaches.
All inputs are finite; a program needn't handle non-finite values.
Results may differ from the reference program's by a relative error of at most 0.017.
Values may be sent and summed in bfloat16 or wider, within the bound.
A program may use at most 128 MiB of HBM per device.

```python
import math
import jax
import jax.numpy as jnp
import numpy as np
from jax import lax

D = 2048
HEADS = 32
BLOCK = 64
LRU = 2048
TAPS = 4
FFE = 3072
DFF = 6144
EXPERTS = 8
TOPK = 2
SEQ_DEV = 64
BATCH = 512
CAP = 18
N_EP = 8
N_TP = 4


def draw_hidden(key, part):
    noise_key = jax.random.fold_in(key, 11)
    column = jnp.arange(D, dtype=jnp.float32) / (D - 1)
    scales = 0.5 * jnp.power(4.0, column)
    values = jax.random.normal(noise_key, (BATCH, D), jnp.float32) * scales[None, :]
    return jnp.clip(values, -10.0, 10.0).astype(jnp.bfloat16)


def shard_levels(rng, shape, cuts, smallest, top_value):
    loudness = 1.0
    for dim, shards_of in cuts:
        draws = jax.random.uniform(jax.random.fold_in(jax.random.fold_in(rng, 6), dim), (shards_of,), jnp.float32, smallest / len(cuts), top_value / len(cuts))
        loudness = loudness * jnp.repeat(jnp.exp(draws), shape[dim] // shards_of).reshape((-1,) + (1,) * (len(shape) - 1 - dim))
    return loudness


def assign_block(key, own, number, rows, count, top, reach, slope):
    sequence = jax.random.permutation(key, count)
    crowded, common = portions_of(count, rows * top, reach, slope, True), portions_of(count, rows * top, reach, slope, False)
    places = jnp.arange(count)

    def named(lengths, turn):
        used = int((lengths > 0).sum())
        fixed = max(1, used // 4)
        passed = fixed + (places - fixed + turn * (used - fixed)) % max(1, count - fixed)
        return jnp.zeros((count,), jnp.int32).at[sequence[jnp.where(places < fixed, places, passed)]].set(jnp.asarray(lengths, jnp.int32))

    lengths = jnp.where(number % 4 == 0, named(crowded, number // 4), named(common, number - number // 4 - 1))
    mixed = jax.random.permutation(jax.random.fold_in(own, 3), count)
    source_of, receiver = mixed[0:count // 2 * 2:2], mixed[1:count // 2 * 2:2]
    margin = jnp.minimum(lengths[source_of] - 1, reach - lengths[receiver]) // 2
    margin = jnp.where((source_of == sequence[0]) | (receiver == sequence[0]) | (lengths[receiver] == 0), 0, jnp.maximum(margin, 0))
    passed = jax.random.randint(jax.random.fold_in(own, 4), (count // 2,), 0, 1 << 20) % (margin + 1)
    lengths = lengths.at[source_of].add(-passed).at[receiver].add(passed)
    labels = jnp.searchsorted(jnp.cumsum(lengths), jnp.arange(rows * top), side="right").astype(jnp.int32)
    listing = labels.reshape(top, rows).T
    listing = listing[jax.random.permutation(jax.random.fold_in(own, 1), rows)]
    turn = jax.random.randint(jax.random.fold_in(own, 2), (rows, 1), 0, top)
    return jnp.take_along_axis(listing, (jnp.arange(top)[None, :] + turn) % top, axis=1)


def portions_of(count, total, limit, lean, full):
    portions = [(1 << 20) // math.isqrt(rank ** lean) + 1 for rank in range(1, count + 1)]
    largest = limit if full else min(limit, max(-(-total // count), total * portions[0] // sum(portions)))
    least = 1 if total - largest >= count - 1 else 0
    counts, rest = [largest] + [least] * (count - 1), total - largest - least * (count - 1)
    while rest > 0:
        movable = [i for i in range(1, count) if counts[i] < largest] or [i for i in range(1, count) if counts[i] < limit]
        whole, budget = sum([portions[i] for i in movable]), rest
        for i in movable:
            addition = min(limit - counts[i], max(1, budget * portions[i] // whole), rest)
            counts[i] = counts[i] + addition
            rest = rest - addition
    return np.array(counts)


def bell_draw(stream_key, dims, spread, reach, split=(), held_as=jnp.bfloat16):
    values = jax.random.normal(stream_key, dims, jnp.float32) * spread
    if len(split) > 0:
        values = shard_levels(stream_key, dims, split, -0.22, 0.18) * values
    return jnp.clip(values, min=-reach, max=reach).astype(held_as)


def setup_inputs(seed: int = 0) -> dict:
    streams_of = jax.random.split(jax.random.key(seed), 22)
    hidden = draw_hidden(jax.random.fold_in(streams_of[21], 71), 0)
    mix_gain = jnp.clip(1.0 + 0.18 * jax.random.normal(streams_of[1], (D,), jnp.float32), 0.099609375, 1.8984375).astype(jnp.bfloat16)
    proj_x = bell_draw(streams_of[2], (D, LRU), D ** -0.5, 0.125, ((0, 8), (1, 4)))
    proj_y = bell_draw(streams_of[3], (D, LRU), D ** -0.5, 0.125, ((0, 8), (1, 4)))
    conv_taps = bell_draw(streams_of[4], (TAPS, LRU), 0.5, 3.0, ((1, 4),))
    input_gate = bell_draw(streams_of[5], (HEADS, BLOCK, BLOCK), BLOCK ** -0.5, 0.75, ((0, 4),))
    decay_gate = bell_draw(streams_of[6], (HEADS, BLOCK, BLOCK), BLOCK ** -0.5, 0.75, ((0, 4),))
    decay_param = jnp.clip(1.0 + 5.0 * jax.random.uniform(streams_of[7], (LRU,), jnp.float32) ** shard_levels(streams_of[7], (LRU,), ((0, 4),), -0.2, 0.2), 1.0, 6.0)
    proj_out = bell_draw(streams_of[8], (LRU, D), LRU ** -0.5, 0.125, ((0, 4),))
    conv_state = bell_draw(streams_of[9], (BATCH, TAPS - 1, LRU), 1.0, 6.0, ((0, 8), (2, 4)))
    lru_state = bell_draw(streams_of[10], (BATCH, LRU), 1.0, 6.0, ((0, 8), (1, 4)), jnp.float32)
    ffn_gain = jnp.clip(1.0 + 0.18 * jax.random.normal(streams_of[11], (D,), jnp.float32), 0.099609375, 1.8984375).astype(jnp.bfloat16)
    routes_keys = jax.random.split(jax.random.fold_in(streams_of[12], 1), BATCH // SEQ_DEV)
    routes_turns = jax.random.permutation(jax.random.fold_in(streams_of[12], 3), BATCH // SEQ_DEV)
    routes = jax.vmap(lambda own, number: assign_block(jax.random.fold_in(streams_of[12], 2), own, number, SEQ_DEV, EXPERTS, TOPK, CAP, 1))(routes_keys, routes_turns).reshape((BATCH, TOPK))
    route_weights = jnp.clip(jnp.exp(math.log(1.0) - 1.609438 * jax.random.uniform(streams_of[13], (BATCH, TOPK), jnp.float32) ** shard_levels(streams_of[13], (BATCH, TOPK), ((0, 8),), -0.2, 0.2)), 0.2, 1.0)
    expert_gate = bell_draw(streams_of[14], (EXPERTS, D, FFE), D ** -0.5, 0.125, ((0, 8), (2, 4)))
    expert_up = bell_draw(streams_of[15], (EXPERTS, D, FFE), D ** -0.5, 0.125, ((0, 8), (2, 4)))
    expert_down = bell_draw(streams_of[16], (EXPERTS, FFE, D), FFE ** -0.5, 0.109375, ((0, 8), (1, 4)))
    dense_gate = bell_draw(streams_of[17], (D, DFF), D ** -0.5, 0.125, ((0, 4), (1, 8)))
    dense_up = bell_draw(streams_of[18], (D, DFF), D ** -0.5, 0.125, ((0, 4), (1, 8)))
    dense_down = bell_draw(streams_of[19], (DFF, D), DFF ** -0.5, 0.078125, ((0, 8), (1, 4)))
    branch_gate = bell_draw(streams_of[20], (D,), 1.0, 4.0, ((0, 4),), jnp.float32)
    return dict(hidden=hidden, mix_gain=mix_gain, proj_x=proj_x, proj_y=proj_y, conv_taps=conv_taps, input_gate=input_gate, decay_gate=decay_gate, decay_param=decay_param, proj_out=proj_out, conv_state=conv_state, lru_state=lru_state, ffn_gain=ffn_gain, routes=routes, route_weights=route_weights, expert_gate=expert_gate, expert_up=expert_up, expert_down=expert_down, dense_gate=dense_gate, dense_up=dense_up, dense_down=dense_down, branch_gate=branch_gate)


epsilon = 1e-06
decay_scale = 8.0

def rms_scale(values, gain_vec):
    floats = values.astype(jnp.float32)
    meansq = lax.optimization_barrier(jnp.mean(floats * floats, axis=-1, keepdims=True))
    return floats * lax.rsqrt(meansq + epsilon) * gain_vec.astype(jnp.float32)

def reference(hidden, mix_gain, proj_x, proj_y, conv_taps, input_gate, decay_gate, decay_param, proj_out, conv_state, lru_state, ffn_gain, routes, route_weights, expert_gate, expert_up, expert_down, dense_gate, dense_up, dense_down, branch_gate):
    batch_rows = hidden.shape[0]
    lru_width = HEADS * BLOCK
    normed = rms_scale(hidden, mix_gain).astype(jnp.bfloat16)
    x_proj = jnp.dot(normed, proj_x, preferred_element_type=jnp.float32).astype(jnp.bfloat16)
    y_proj = jnp.dot(normed, proj_y, preferred_element_type=jnp.float32).astype(jnp.bfloat16)
    window = jnp.concatenate([conv_state, x_proj[:, None, :]], axis=1)
    conv_out = lax.optimization_barrier(jnp.sum(window.astype(jnp.float32) * conv_taps.astype(jnp.float32)[None], axis=1)).astype(jnp.bfloat16)
    heads_in = conv_out.astype(jnp.float32).reshape(batch_rows, HEADS, BLOCK)
    gate_in = jax.nn.sigmoid(jnp.einsum('bhi,hij->bhj', heads_in, input_gate.astype(jnp.float32)).reshape(batch_rows, lru_width))
    gate_dec = jax.nn.sigmoid(jnp.einsum('bhi,hij->bhj', heads_in, decay_gate.astype(jnp.float32)).reshape(batch_rows, lru_width))
    log_decay = decay_scale * gate_dec * jax.nn.log_sigmoid(decay_param)
    decay_rate = jnp.exp(log_decay)
    inject = jnp.sqrt(-jnp.expm1(2.0 * log_decay))
    new_lru = decay_rate * lru_state + inject * gate_in * conv_out.astype(jnp.float32)
    gated_out = (new_lru * jax.nn.gelu(y_proj.astype(jnp.float32))).astype(jnp.bfloat16)
    head_share = lru_width // N_TP
    mixer_sum = jnp.zeros((batch_rows, D), jnp.float32)
    for member in range(N_TP):
        partial_value = jnp.dot(gated_out[:, member * head_share:(member + 1) * head_share], proj_out[member * head_share:(member + 1) * head_share], preferred_element_type=jnp.float32).astype(jnp.bfloat16)
        mixer_sum = mixer_sum + partial_value.astype(jnp.float32)
    summed = (hidden.astype(jnp.float32) + mixer_sum).astype(jnp.bfloat16)
    ffn_in = rms_scale(summed, ffn_gain).astype(jnp.bfloat16)
    pair_expert = routes.reshape(-1).astype(jnp.int32)
    onehot = (pair_expert[:, None] == jnp.arange(EXPERTS, dtype=jnp.int32)[None, :]).astype(jnp.int32)
    grouped = onehot.reshape(N_EP, SEQ_DEV * TOPK, EXPERTS)
    before = jnp.cumsum(grouped, axis=1) - grouped
    slot_rank = lax.optimization_barrier(jnp.sum(before * grouped, axis=2)).reshape(-1)
    group_of = jnp.arange(BATCH * TOPK, dtype=jnp.int32) // (SEQ_DEV * TOPK)
    position = (group_of * CAP + slot_rank).astype(jnp.int32)
    token_of = jnp.arange(BATCH * TOPK, dtype=jnp.int32) // TOPK
    buffer = jnp.zeros((EXPERTS, N_EP * CAP, D), jnp.bfloat16).at[pair_expert, position].set(ffn_in[token_of])
    ff_share = FFE // N_TP

    def one_expert(operands):
        slot_rows, gate_w, up_w, down_w = operands
        gate_val = jnp.dot(slot_rows, gate_w, preferred_element_type=jnp.float32)
        up_val = jnp.dot(slot_rows, up_w, preferred_element_type=jnp.float32)
        inner_act = (jax.nn.silu(gate_val) * up_val).astype(jnp.bfloat16)
        total_out = jnp.zeros((slot_rows.shape[0], D), jnp.float32)
        for member in range(N_TP):
            piece_out = jnp.dot(inner_act[:, member * ff_share:(member + 1) * ff_share], down_w[member * ff_share:(member + 1) * ff_share], preferred_element_type=jnp.float32).astype(jnp.bfloat16)
            total_out = total_out + piece_out.astype(jnp.float32)
        return total_out.astype(jnp.bfloat16)
    results = lax.map(one_expert, (buffer, expert_gate, expert_up, expert_down))
    picked = results[pair_expert, position].astype(jnp.float32)
    expert_sum = lax.optimization_barrier(jnp.sum((picked * route_weights.reshape(-1)[:, None]).reshape(batch_rows, TOPK, D), axis=1))
    dense_g = jnp.dot(ffn_in, dense_gate, preferred_element_type=jnp.float32)
    dense_u = jnp.dot(ffn_in, dense_up, preferred_element_type=jnp.float32)
    dense_hid = (jax.nn.silu(dense_g) * dense_u).astype(jnp.bfloat16)
    dense_out = jnp.dot(dense_hid, dense_down, preferred_element_type=jnp.float32)
    new_hidden = (summed.astype(jnp.float32) + expert_sum + jax.nn.sigmoid(branch_gate)[None, :] * dense_out).astype(jnp.bfloat16)
    return (new_hidden, new_lru, window[:, 1:])
```

```python
import functools

import jax
import jax.numpy as jnp
from jax import lax
from jax.experimental import pallas as pl
from jax.experimental.pallas import tpu as pltpu
from jax.sharding import PartitionSpec as P

epsilon = 1e-06
decay_scale = 8.0
MESH = pl.DeviceIdType.MESH
F32 = jnp.float32
BF16 = jnp.bfloat16


def rms_scale(values, gain_vec):
    floats = values.astype(F32)
    meansq = jnp.mean(floats * floats, axis=-1, keepdims=True)
    return floats * lax.rsqrt(meansq + epsilon) * gain_vec.astype(F32)


def dot(a, b):
    return jnp.dot(a, b, preferred_element_type=F32)


def layer_kernel(
    E, T, slots,
    nb, ct, hid_own, wx, wy, conv_pre, tap_new, bd, log_dec, lru, gain_own, branch,
    po_h, dwp_h, eg_h, eu_h, ed_h, dd_h,
    new_hidden, new_lru, x_out,
    po, eg, eu, ed, dd, dwr, spread, pbuf, parts, ctr, acc, mbuf, mrec, qbuf, qrec,
    xall, hacc, aall, xe, hid, sel, ebuf, erec, obuf, orec, summed_ref,
    load_sem, nb_s, nb_r, ct_s, ct_r, pt_s, pt_r, dw_s, dw_r, mx_s, mx_r, q_s, q_r,
    xe_s, x2_s, x1_s, x_r, a_s, a_r, er_s, er_r, o_s, o_r,
):
    e = lax.axis_index("ep")
    t = lax.axis_index("tp")
    M, C = hid_own.shape
    D = C * T

    def ep_peer(k):
        return lax.rem(e + k, E)

    def ep_from(k):
        return lax.rem(e + E - k, E)

    def tp_peer(k):
        return lax.rem(t + k, T)

    across = lax.rem(t + T // 2, T)
    beside = t + 1 - 2 * lax.rem(t, 2)
    diagonal = lax.rem(beside + T // 2, T)

    loads = [
        pltpu.make_async_copy(src, dst, load_sem.at[i])
        for i, (src, dst) in enumerate(
            ((po_h, po), (eg_h, eg), (eu_h, eu), (ed_h, ed), (dd_h, dd))
        )
    ]
    own_dw = pltpu.make_async_copy(dwp_h.at[t], dwr.at[t], load_sem.at[5])

    def rcopy(src, dst, s, r, ep=None, tp=None):
        return pltpu.make_async_remote_copy(
            src_ref=src, dst_ref=dst, send_sem=s, recv_sem=r,
            device_id=(e if ep is None else ep, t if tp is None else tp),
            device_id_type=MESH,
        )

    barrier = pltpu.get_barrier_semaphore()

    @pl.loop(1, E)
    def _(k):
        pl.semaphore_signal(barrier, inc=1, device_id=(ep_peer(k), t), device_id_type=MESH)

    for k in range(1, T):
        pl.semaphore_signal(barrier, inc=1, device_id=(e, tp_peer(k)), device_id_type=MESH)
    pl.semaphore_wait(barrier, E - 1 + T - 1)

    @pl.loop(1, E)
    def _(k):
        p = ep_peer(k)
        rcopy(nb.at[p], spread.at[e], nb_s.at[p], nb_r.at[e], ep=p).start()
        rcopy(ct.at[p], ctr.at[e], ct_s.at[p], ct_r.at[e], ep=p).start()

    loads[0].start()
    own_dw.start()
    for k in range(1, T):
        j = tp_peer(k)
        rcopy(dwp_h.at[j], dwr.at[t], dw_s.at[j], dw_r.at[t], tp=j).start()
    for l in loads[1:]:
        l.start()

    acc[:, :C] = dot(nb[e], wx[...])
    acc[:, C:] = dot(nb[e], wy[...])

    @pl.loop(1, E)
    def _(k):
        s = ep_from(k)
        rcopy(nb.at[s], spread.at[s], nb_s.at[s], nb_r.at[s], ep=s).wait_recv()
        blk = spread[s]
        pbuf[s, :, :C] = dot(blk, wx[...]).astype(BF16)
        pbuf[s, :, C:] = dot(blk, wy[...]).astype(BF16)
        rcopy(pbuf.at[s], parts.at[e], pt_s.at[s], pt_r.at[e], ep=s).start()

    @pl.loop(1, E)
    def _(k):
        s = ep_from(k)
        rcopy(ct.at[s], ctr.at[s], ct_s.at[s], ct_r.at[s], ep=s).wait_recv()

    ctr[e] = ct[e]
    N = E * M
    w_row = ctr[0]
    for s in range(1, E):
        w_row = w_row + ctr[s]
    nblk = min(N, 512)
    tri = (
        lax.broadcasted_iota(jnp.int32, (nblk, nblk), 0)
        < lax.broadcasted_iota(jnp.int32, (nblk, nblk), 1)
    ).astype(F32).astype(BF16)
    base = jnp.zeros((1, 1), F32)
    w_slot = jnp.zeros((slots, 1), F32)
    for b in range(N // nblk):
        w_b = w_row[:, b * nblk:(b + 1) * nblk]
        m_b = (w_b > 0.0).astype(F32)
        rank = dot(jnp.broadcast_to(m_b, (16, nblk)).astype(BF16), tri)[0:1, :] + base
        base = base + jnp.sum(m_b, axis=1, keepdims=True)
        hit = (
            lax.broadcasted_iota(jnp.int32, (slots, nblk), 0).astype(F32) == rank
        ).astype(F32) * m_b
        sel[:, b * nblk:(b + 1) * nblk] = hit.astype(BF16)
        w_slot = w_slot + jnp.sum(hit * w_b, axis=1, keepdims=True)

    @pl.loop(1, E)
    def _(k):
        p = ep_peer(k)
        rcopy(pbuf.at[p], parts.at[p], pt_s.at[p], pt_r.at[p], ep=p).wait_recv()
        acc[...] += parts[p].astype(F32)

    x_b = acc[:, :C].astype(BF16)
    y_b = acc[:, C:].astype(BF16)
    x_out[...] = x_b
    conv = (conv_pre[...] + x_b.astype(F32) * tap_new[...]).astype(BF16)
    width = bd.shape[1]
    gi, gd = [], []
    for i in range(C // width):
        g = dot(conv[:, i * width:(i + 1) * width], bd[i])
        gi.append(g[:, :width])
        gd.append(g[:, width:])
    gate_in = jax.nn.sigmoid(jnp.concatenate(gi, axis=1))
    gate_dec = jax.nn.sigmoid(jnp.concatenate(gd, axis=1))
    log_decay = gate_dec * log_dec[...]
    decay = jnp.exp(log_decay)
    inject = jnp.sqrt(-jnp.tanh(log_decay) * (1.0 + decay * decay))
    state = decay * lru[...] + inject * gate_in * conv.astype(F32)
    new_lru[...] = state
    gated = (state * jax.nn.gelu(y_b.astype(F32), approximate=True)).astype(BF16)

    loads[0].wait()
    order = [tp_peer(k) for k in (2, 3, 1)] if T == 4 else [tp_peer(k) for k in range(1, T)]
    for j in order:
        cols = pl.ds(pl.multiple_of(j * C, 128), C)
        mbuf[j] = dot(gated, po[:, cols]).astype(BF16)
        rcopy(mbuf.at[j], mrec.at[t], mx_s.at[j], mx_r.at[t], tp=j).start()
    own_cols = pl.ds(pl.multiple_of(t * C, 128), C)
    mixer = dot(gated, po[:, own_cols]).astype(BF16).astype(F32)
    for j in reversed(order):
        rcopy(mbuf.at[j], mrec.at[j], mx_s.at[j], mx_r.at[j], tp=j).wait_recv()
        mixer = mixer + mrec[j].astype(F32)
    summed = (hid_own[...].astype(F32) + mixer).astype(BF16)
    summed_ref[...] = summed
    sf = summed.astype(F32)
    ssq = jnp.sum(sf * sf, axis=1, keepdims=True)
    qbuf[...] = jnp.broadcast_to(ssq, qbuf.shape)
    for j in order:
        rcopy(qbuf, qrec.at[t], q_s.at[j], q_r.at[t], tp=j).start()
    total = qbuf[...]
    for j in reversed(order):
        rcopy(qbuf, qrec.at[j], q_s.at[j], q_r.at[j], tp=j).wait_recv()
        total = total + qrec[j]
    scale = lax.rsqrt(total[:, 0:1] * (1.0 / D) + epsilon)
    xall[t, e] = (sf * scale * gain_own[...]).astype(BF16)

    @pl.loop(1, E)
    def _(k):
        p = ep_peer(k)
        rcopy(xall.at[t, e], xall.at[t, e], xe_s.at[p], x_r.at[t, e], ep=p).start()

    def spread_tp(s):
        rcopy(xall.at[t, s], xall.at[t, s], x2_s.at[s], x_r.at[t, s], tp=across).start()
        rcopy(xall.at[t, s], xall.at[t, s], x1_s.at[0, s], x_r.at[t, s], tp=beside).start()

    def forward(s):
        rcopy(xall.at[across, s], xall.at[across, s], x2_s.at[s], x_r.at[across, s], tp=across).wait_recv()
        rcopy(xall.at[across, s], xall.at[across, s], x1_s.at[1, s], x_r.at[across, s], tp=beside).start()

    spread_tp(e)

    @pl.loop(1, E)
    def _(k):
        s = ep_from(k)
        rcopy(xall.at[t, s], xall.at[t, s], xe_s.at[s], x_r.at[t, s], ep=s).wait_recv()
        spread_tp(s)
        forward(ep_from(k - 1))

    forward(ep_from(E - 1))

    @pl.loop(0, E)
    def _(s):
        rcopy(xall.at[beside, s], xall.at[beside, s], x1_s.at[0, s], x_r.at[beside, s], tp=beside).wait_recv()
        rcopy(xall.at[diagonal, s], xall.at[diagonal, s], x1_s.at[1, s], x_r.at[diagonal, s], tp=beside).wait_recv()

    own_dw.wait()
    for j in order:
        rcopy(dwp_h.at[j], dwr.at[j], dw_s.at[j], dw_r.at[j], tp=j).wait_recv()
    rows = min(N, 512)

    @pl.loop(0, N // rows)
    def _(b):
        hacc[...] = jnp.zeros_like(hacc)
        eb = rows // M

        @pl.loop(0, T)
        def _(q):
            xq = xall[q, pl.ds(b * eb, eb)].reshape(rows, C)
            hacc[...] += dot(xq, dwr[q])

        h = hacc[...]
        half = h.shape[1] // 2
        act = jax.nn.silu(h) * pltpu.roll(h, half, axis=1)
        aall[t, pl.ds(pl.multiple_of(b * rows, 16), rows), :] = act[:, :half].astype(BF16)

    a_across = rcopy(aall.at[t], aall.at[t], a_s.at[0], a_r.at[t], tp=across)
    a_beside = rcopy(aall.at[t], aall.at[t], a_s.at[1], a_r.at[t], tp=beside)
    a_across.start()
    a_beside.start()

    @pl.loop(0, T)
    def _(q):
        cols = pl.ds(pl.multiple_of(q * C, 128), C)
        xe[:, cols] = dot(sel[...], xall[q].reshape(N, C)).astype(BF16)

    loads[1].wait()
    loads[2].wait()
    FH = eg.shape[1]
    nch = 256 if FH % 256 == 0 else FH

    @pl.loop(0, FH // nch)
    def _(n):
        cols = pl.ds(pl.multiple_of(n * nch, 128), nch)
        g = dot(xe[...], eg[:, cols])
        u = dot(xe[...], eu[:, cols])
        hid[:, cols] = (jax.nn.silu(g) * u).astype(BF16)

    a_in = rcopy(aall.at[across], aall.at[across], a_s.at[0], a_r.at[across], tp=across)
    a_in.wait_recv()
    a_fwd = rcopy(aall.at[across], aall.at[across], a_s.at[2], a_r.at[across], tp=beside)
    a_fwd.start()

    loads[3].wait()
    for j in order:
        cols = pl.ds(pl.multiple_of(j * C, 128), C)
        ebuf[j] = dot(hid[...], ed[:, cols]).astype(BF16)
        rcopy(ebuf.at[j], erec.at[t], er_s.at[j], er_r.at[t], tp=j).start()
    ebuf[t] = dot(hid[...], ed[:, own_cols]).astype(BF16)

    loads[4].wait()
    rcopy(aall.at[beside], aall.at[beside], a_s.at[1], a_r.at[beside], tp=beside).wait_recv()
    rcopy(aall.at[diagonal], aall.at[diagonal], a_s.at[2], a_r.at[diagonal], tp=beside).wait_recv()
    red = ebuf[t].astype(F32)
    for j in reversed(order):
        rcopy(ebuf.at[j], erec.at[j], er_s.at[j], er_r.at[j], tp=j).wait_recv()
        red = red + erec[j].astype(F32)
    red = (red.astype(BF16).astype(F32) * w_slot).astype(BF16)
    gate = jax.nn.sigmoid(branch[...])
    ob = 128 if N % 128 == 0 else M
    ebuf[t] = red

    @pl.loop(0, N // ob)
    def _(b):
        rws = pl.ds(pl.multiple_of(b * ob, 128 if ob % 128 == 0 else 16), ob)
        d = dot(aall[0, rws, :], dd[0])
        for q in range(1, T):
            d = d + dot(aall[q, rws, :], dd[q])
        d = d * gate + lax.dot_general(
            sel[:, rws], ebuf[t], (((0,), (0,)), ((), ())), preferred_element_type=F32
        )
        obuf[pl.ds(b * (ob // M), ob // M)] = d.reshape(ob // M, M, C).astype(BF16)

    @pl.loop(1, E)
    def _(k):
        p = ep_peer(k)
        rcopy(obuf.at[p], orec.at[e], o_s.at[p], o_r.at[e], ep=p).start()

    acc[:, :C] = summed_ref[...].astype(F32) + obuf[e].astype(F32)

    @pl.loop(1, E)
    def _(k):
        s = ep_from(k)
        rcopy(obuf.at[s], orec.at[s], o_s.at[s], o_r.at[s], ep=s).wait_recv()
        acc[:, :C] += orec[s].astype(F32)

    new_hidden[...] = acc[:, :C].astype(BF16)

    @pl.loop(1, E)
    def _(k):
        p = ep_peer(k)
        rcopy(nb.at[p], spread.at[e], nb_s.at[p], nb_r.at[e], ep=p).wait_send()
        rcopy(ct.at[p], ctr.at[e], ct_s.at[p], ct_r.at[e], ep=p).wait_send()
        rcopy(pbuf.at[p], parts.at[e], pt_s.at[p], pt_r.at[e], ep=p).wait_send()
        rcopy(xall.at[t, e], xall.at[t, e], xe_s.at[p], x_r.at[t, e], ep=p).wait_send()
        rcopy(obuf.at[p], orec.at[e], o_s.at[p], o_r.at[e], ep=p).wait_send()

    for j in order:
        rcopy(dwp_h.at[j], dwr.at[t], dw_s.at[j], dw_r.at[t], tp=j).wait_send()
        rcopy(mbuf.at[j], mrec.at[t], mx_s.at[j], mx_r.at[t], tp=j).wait_send()
        rcopy(qbuf, qrec.at[t], q_s.at[j], q_r.at[t], tp=j).wait_send()
        rcopy(ebuf.at[j], erec.at[t], er_s.at[j], er_r.at[t], tp=j).wait_send()

    @pl.loop(0, E)
    def _(s):
        rcopy(xall.at[t, s], xall.at[t, s], x2_s.at[s], x_r.at[t, s], tp=across).wait_send()
        rcopy(xall.at[t, s], xall.at[t, s], x1_s.at[0, s], x_r.at[t, s], tp=beside).wait_send()
        rcopy(xall.at[across, s], xall.at[across, s], x1_s.at[1, s], x_r.at[across, s], tp=beside).wait_send()

    a_across.wait_send()
    a_beside.wait_send()
    a_fwd.wait_send()


def on_device(
    hidden, mix_gain, proj_x, proj_y, conv_taps, input_gate, decay_gate, decay_param,
    proj_out, conv_state, lru_state, ffn_gain, routes, route_weights,
    expert_gate, expert_up, expert_down, dense_gate, dense_up, dense_down, branch_gate,
):
    E = lax.axis_size("ep")
    T = lax.axis_size("tp")
    e = lax.axis_index("ep")
    t = lax.axis_index("tp")
    M, D = hidden.shape
    C = D // T
    R = proj_x.shape[0]
    N = E * M
    normed = rms_scale(hidden, mix_gain).astype(BF16)
    nb = normed.reshape(M, E, R).transpose(1, 0, 2)
    hid_own = lax.dynamic_slice_in_dim(hidden, t * C, C, 1)
    gain_own = lax.dynamic_slice_in_dim(ffn_gain, t * C, C, 0).astype(F32)[None, :]
    taps = conv_taps.astype(F32)
    conv_pre = jnp.sum(conv_state.astype(F32) * taps[None, :-1], axis=1)
    heads, block = input_gate.shape[:2]
    group = max(1, 128 // block)

    def diag(g):
        g = g.reshape(heads // group, group, block, 1, block)
        eye = jnp.eye(group, dtype=g.dtype).reshape(1, group, 1, group, 1)
        return (g * eye).reshape(heads // group, group * block, group * block)

    bd = jnp.concatenate([diag(input_gate), diag(decay_gate)], axis=2)
    log_dec = (decay_scale * jax.nn.log_sigmoid(decay_param))[None, :]
    experts = expert_gate.shape[0] * E
    ids = jnp.arange(experts, dtype=jnp.int32)
    rows_w = jnp.sum(
        jnp.where(routes.T[None, :, :] == ids[:, None, None], route_weights.T[None], 0.0), axis=1
    )
    here = (jnp.arange(E) == e).astype(F32)
    ct = (here[None, :, None] * rows_w[:, None, :]).reshape(experts, 1, N)
    capacity = M * routes.shape[1] // experts + 2
    slots = -(-E * capacity // 16) * 16
    h = dense_gate.shape[1] // T
    half = -(-2 * h // 128) * 64

    def cut(w):
        w = w.reshape(C, T, h).transpose(1, 0, 2)
        return jnp.pad(w, ((0, 0), (0, 0), (0, half - h)))

    dwp = jnp.concatenate([cut(dense_gate), cut(dense_up)], axis=2)
    dd = jnp.pad(dense_down.reshape(T, h, C), ((0, 0), (0, half - h), (0, 0)))
    FH = expert_gate.shape[2]
    vm = pl.BlockSpec(memory_space=pltpu.VMEM)
    anyspace = pl.BlockSpec(memory_space=pl.ANY)
    DMA = pltpu.SemaphoreType.DMA
    V = pltpu.VMEM
    rows = min(N, 512)
    scratch = [
        V((C, D), BF16), V((D, FH), BF16), V((D, FH), BF16), V((FH, D), BF16), V((T, half, C), BF16),
        V((T, C, 2 * half), BF16),
        V((E, M, R), BF16), V((E, M, 2 * C), BF16), V((E, M, 2 * C), BF16), V((E, 1, N), F32),
        V((M, 2 * C), F32),
        V((T, M, C), BF16), V((T, M, C), BF16), V((M, 128), F32), V((T, M, 128), F32),
        V((T, E, M, C), BF16), V((rows, 2 * half), F32), V((T, N, half), BF16),
        V((slots, D), BF16), V((slots, FH), BF16), V((slots, N), BF16),
        V((T, slots, C), BF16), V((T, slots, C), BF16), V((E, M, C), BF16), V((E, M, C), BF16),
        V((M, C), BF16),
        DMA((6,)),
        DMA((E,)), DMA((E,)), DMA((E,)), DMA((E,)), DMA((E,)), DMA((E,)),
        DMA((T,)), DMA((T,)), DMA((T,)), DMA((T,)), DMA((T,)), DMA((T,)),
        DMA((E,)), DMA((E,)), DMA((2, E)), DMA((T, E)), DMA((3,)), DMA((T,)), DMA((T,)), DMA((T,)),
        DMA((E,)), DMA((E,)),
    ]
    new_hidden, new_lru, x_new = pl.pallas_call(
        functools.partial(layer_kernel, E, T, slots),
        out_shape=(
            jax.ShapeDtypeStruct((M, C), BF16),
            jax.ShapeDtypeStruct((M, C), F32),
            jax.ShapeDtypeStruct((M, C), BF16),
        ),
        in_specs=[vm] * 12 + [anyspace] * 6,
        out_specs=(vm, vm, vm),
        scratch_shapes=scratch,
        compiler_params=pltpu.CompilerParams(
            collective_id=0, has_side_effects=True, vmem_limit_bytes=60 * 1024 * 1024
        ),
    )(
        nb, ct, hid_own, proj_x, proj_y, conv_pre, taps[-1:], bd, log_dec, lru_state, gain_own,
        branch_gate[None, :], proj_out, dwp, expert_gate[0], expert_up[0], expert_down[0], dd,
    )
    new_conv = jnp.concatenate([conv_state[:, 1:], x_new[:, None, :]], axis=1)
    return (new_hidden, new_lru, new_conv)


def solution(mesh):
    in_specs = (
        P("ep", None),
        P(),
        P("ep", "tp"),
        P("ep", "tp"),
        P(None, "tp"),
        P("tp", None, None),
        P("tp", None, None),
        P("tp"),
        P("tp", None),
        P("ep", None, "tp"),
        P("ep", "tp"),
        P(),
        P("ep", None),
        P("ep", None),
        P("ep", None, "tp"),
        P("ep", None, "tp"),
        P("ep", "tp", None),
        P("tp", "ep"),
        P("tp", "ep"),
        P("ep", "tp"),
        P("tp"),
    )
    out_specs = (P("ep", "tp"), P("ep", "tp"), P("ep", None, "tp"))
    return jax.shard_map(
        on_device, mesh=mesh, in_specs=in_specs, out_specs=out_specs, check_vma=False
    )
```

```python
import functools

import jax
import jax.numpy as jnp
from jax import lax
from jax.experimental import pallas as pl
from jax.experimental.pallas import tpu as pltpu
from jax.sharding import PartitionSpec as P

epsilon = 1e-06
decay_scale = 8.0
MESH = pl.DeviceIdType.MESH
F32 = jnp.float32
BF16 = jnp.bfloat16


def dot(a, b):
    return jnp.dot(a, b, preferred_element_type=F32)


def layer_kernel(
    E, T, slots,
    hidden, mix_gain, routes, weights, conv_old, taps, ig, dgate, decay_param, lru, ffn_gain, branch,
    wx_h, wy_h, dg_h, du_h, po_h, eg_h, eu_h, ed_h, dd_h,
    new_hidden, new_lru, x_out,
    ct, w_ref, bd, wx, wy, dg, du, po, eg, eu, ed, dd, nb, dwp, dwr, spread, pm, pacc, yrec, zout, zrec, ctr, acc,
    mbuf, mrec, qbuf, qrec, xall, hacc, aall, xe, hid, sel, ebuf, erec, dtmp, om, dacc, orm, oz, ozr,
    summed_ref,
    load_sem, nb_s, nb_r, ct_s, ct_r, pm_s, pm_r, pz_s, pz_r, dw_s, dw_r, mx_s, mx_r, q_s, q_r,
    xr_s, xm_s, x2_s, x1_s, x_r, a_s, a_r, er_s, er_r, om_s, om_r, oz_s, oz_r,
):
    e = lax.axis_index("ep")
    t = lax.axis_index("tp")
    M, D = hidden.shape
    C = D // T
    R = wx.shape[0]
    G = E // 2
    g0 = e // 2
    par = lax.rem(e, 2)
    mate = e + 1 - 2 * par
    own_cols = pl.ds(pl.multiple_of(t * C, 128), C)

    def ep_peer(k):
        return lax.rem(e + k, E)

    def ep_from(k):
        return lax.rem(e + E - k, E)

    def group(k):
        return lax.rem(g0 + k, G)

    def rail_from(k):
        return 2 * lax.rem(g0 + G - k, G) + par

    def mate_of(s):
        return s + 1 - 2 * lax.rem(s, 2)

    def tp_peer(k):
        return lax.rem(t + k, T)

    across = lax.rem(t + T // 2, T)
    beside = t + 1 - 2 * lax.rem(t, 2)
    diagonal = lax.rem(beside + T // 2, T)

    loads = [
        pltpu.make_async_copy(src, dst, load_sem.at[i])
        for i, (src, dst) in enumerate(
            ((po_h, po), (eg_h, eg), (eu_h, eu), (ed_h, ed), (dd_h, dd),
             (wx_h, wx), (wy_h, wy), (dg_h, dg), (du_h, du))
        )
    ]
    own_dw = pltpu.make_async_copy(dwp.at[t], dwr.at[t], load_sem.at[9])
    for i in (5, 6, 7, 8, 0):
        loads[i].start()

    def rcopy(src, dst, s, r, ep=None, tp=None):
        return pltpu.make_async_remote_copy(
            src_ref=src, dst_ref=dst, send_sem=s, recv_sem=r,
            device_id=(e if ep is None else ep, t if tp is None else tp),
            device_id_type=MESH,
        )

    barrier = pltpu.get_barrier_semaphore()

    @pl.loop(1, E)
    def _(k):
        pl.semaphore_signal(barrier, inc=1, device_id=(ep_peer(k), t), device_id_type=MESH)

    for k in range(1, T):
        pl.semaphore_signal(barrier, inc=1, device_id=(e, tp_peer(k)), device_id_type=MESH)
    hf = hidden[...].astype(F32)
    inv = lax.rsqrt(jnp.mean(hf * hf, axis=-1, keepdims=True) + epsilon)
    normed = (hf * inv * mix_gain[...].astype(F32)).astype(BF16)
    for p in range(E):
        nb[p] = normed[:, p * R:(p + 1) * R]
    for p in range(E):
        ct[p] = jnp.sum(jnp.where(routes[...] == p, weights[...], 0.0), axis=0, keepdims=True)
    pl.semaphore_wait(barrier, E - 1 + T - 1)

    @pl.loop(1, E)
    def _(k):
        p = ep_peer(k)
        rcopy(nb.at[p], spread.at[e], nb_s.at[p], nb_r.at[e], ep=p).start()
        rcopy(ct.at[p], ctr.at[e], ct_s.at[p], ct_r.at[e], ep=p).start()

    loads[7].wait()
    loads[8].wait()
    h = dg.shape[1] // T
    half = dwp.shape[2] // 2
    if half != h:
        dwp[...] = jnp.zeros_like(dwp)
    for j in range(T):
        dwp[j, :, :h] = dg[:, j * h:(j + 1) * h]
        dwp[j, :, half:half + h] = du[:, j * h:(j + 1) * h]
    own_dw.start()
    for k in range(1, T):
        j = tp_peer(k)
        rcopy(dwp.at[j], dwr.at[t], dw_s.at[j], dw_r.at[t], tp=j).start()
    for l in loads[1:5]:
        l.start()

    spread[e] = nb[e]
    loads[5].wait()
    loads[6].wait()

    def arrive(s):
        rcopy(nb.at[s], spread.at[s], nb_s.at[s], nb_r.at[s], ep=s).wait_recv()

    def share(g):
        blk = spread[2 * g + 1 - par]
        pm[g, :, :C] = dot(blk, wx[...]).astype(BF16)
        pm[g, :, C:] = dot(blk, wy[...]).astype(BF16)
        rcopy(pm.at[g], yrec.at[g], pm_s.at[g], pm_r.at[g], ep=mate).start()
        blk = spread[2 * g + par]
        pacc[g, :, :C] = dot(blk, wx[...])
        pacc[g, :, C:] = dot(blk, wy[...])

    def pass_on(g):
        rcopy(pm.at[g], yrec.at[g], pm_s.at[g], pm_r.at[g], ep=mate).wait_recv()
        zout[g] = (pacc[g] + yrec[g].astype(F32)).astype(BF16)
        rcopy(zout.at[g], zrec.at[g0], pz_s.at[g], pz_r.at[g0], ep=2 * g + par).start()

    @pl.loop(1, G)
    def _(k):
        g = group(k)
        arrive(2 * g + 1 - par)
        arrive(2 * g + par)
        share(g)

        @pl.when(k > 1)
        def _():
            pass_on(group(k - 1))

    arrive(mate)
    share(g0)
    pass_on(group(G - 1))

    @pl.loop(1, E)
    def _(k):
        s = ep_from(k)
        rcopy(ct.at[s], ctr.at[s], ct_s.at[s], ct_r.at[s], ep=s).wait_recv()

    ctr[e] = ct[e]
    N = E * M
    for s in range(E):
        w_ref[:, s * M:(s + 1) * M] = ctr[s]
    w_row = w_ref[...]
    bd[...] = jnp.zeros_like(bd)
    block = ig.shape[1]
    width = bd.shape[1]
    per = width // block
    for i in range(ig.shape[0]):
        lo = i % per * block
        bd[i // per, lo:lo + block, lo:lo + block] = ig[i]
        bd[i // per, lo:lo + block, width + lo:width + lo + block] = dgate[i]
    nblk = min(N, 512)
    tri = (
        lax.broadcasted_iota(jnp.int32, (nblk, nblk), 0)
        < lax.broadcasted_iota(jnp.int32, (nblk, nblk), 1)
    ).astype(F32).astype(BF16)
    base = jnp.zeros((1, 1), F32)
    w_slot = jnp.zeros((slots, 1), F32)
    for b in range(N // nblk):
        w_b = w_row[:, b * nblk:(b + 1) * nblk]
        m_b = (w_b > 0.0).astype(F32)
        rank = dot(jnp.broadcast_to(m_b, (16, nblk)).astype(BF16), tri)[0:1, :] + base
        base = base + jnp.sum(m_b, axis=1, keepdims=True)
        hit = (
            lax.broadcasted_iota(jnp.int32, (slots, nblk), 0).astype(F32) == rank
        ).astype(F32) * m_b
        sel[:, b * nblk:(b + 1) * nblk] = hit.astype(BF16)
        w_slot = w_slot + jnp.sum(hit * w_b, axis=1, keepdims=True)

    rcopy(pm.at[g0], yrec.at[g0], pm_s.at[g0], pm_r.at[g0], ep=mate).wait_recv()
    acc[...] = pacc[g0] + yrec[g0].astype(F32)

    @pl.loop(1, G)
    def _(k):
        g = group(k)
        rcopy(zout.at[g], zrec.at[g], pz_s.at[g], pz_r.at[g], ep=2 * g + par).wait_recv()
        acc[...] += zrec[g].astype(F32)

    x_b = acc[:, :C].astype(BF16)
    y_b = acc[:, C:].astype(BF16)
    x_out[...] = x_b
    conv_pre = conv_old[0].astype(F32) * taps[0:1, :].astype(F32)
    for i in range(1, taps.shape[0] - 1):
        conv_pre = conv_pre + conv_old[i].astype(F32) * taps[i:i + 1, :].astype(F32)
    conv = (conv_pre + x_b.astype(F32) * taps[taps.shape[0] - 1:, :].astype(F32)).astype(BF16)
    gi, gd = [], []
    for i in range(C // width):
        g = dot(conv[:, i * width:(i + 1) * width], bd[i])
        gi.append(g[:, :width])
        gd.append(g[:, width:])
    gate_in = jax.nn.sigmoid(jnp.concatenate(gi, axis=1))
    gate_dec = jax.nn.sigmoid(jnp.concatenate(gd, axis=1))
    dp = decay_param[...]
    log_decay = decay_scale * gate_dec * (jnp.minimum(dp, 0.0) - jnp.log1p(jnp.exp(-jnp.abs(dp))))
    decay = jnp.exp(log_decay)
    inject = jnp.sqrt(-jnp.tanh(log_decay) * (1.0 + decay * decay))
    state = decay * lru[...] + inject * gate_in * conv.astype(F32)
    new_lru[...] = state
    gated = (state * jax.nn.gelu(y_b.astype(F32), approximate=True)).astype(BF16)

    loads[0].wait()
    order = [tp_peer(k) for k in (2, 3, 1)] if T == 4 else [tp_peer(k) for k in range(1, T)]
    for j in order:
        cols = pl.ds(pl.multiple_of(j * C, 128), C)
        mbuf[j] = dot(gated, po[:, cols]).astype(BF16)
        rcopy(mbuf.at[j], mrec.at[t], mx_s.at[j], mx_r.at[t], tp=j).start()
    mixer = dot(gated, po[:, own_cols]).astype(BF16).astype(F32)
    for j in reversed(order):
        rcopy(mbuf.at[j], mrec.at[j], mx_s.at[j], mx_r.at[j], tp=j).wait_recv()
        mixer = mixer + mrec[j].astype(F32)
    summed = (hidden[:, own_cols].astype(F32) + mixer).astype(BF16)
    summed_ref[...] = summed
    sf = summed.astype(F32)
    ssq = jnp.sum(sf * sf, axis=1, keepdims=True)
    qbuf[...] = jnp.broadcast_to(ssq, qbuf.shape)
    for j in order:
        rcopy(qbuf, qrec.at[t], q_s.at[j], q_r.at[t], tp=j).start()
    total = qbuf[...]
    for j in reversed(order):
        rcopy(qbuf, qrec.at[j], q_s.at[j], q_r.at[j], tp=j).wait_recv()
        total = total + qrec[j]
    scale = lax.rsqrt(total[:, 0:1] * (1.0 / D) + epsilon)
    xall[t, e] = (sf * scale * ffn_gain[:, own_cols].astype(F32)).astype(BF16)

    def to_mate(s):
        rcopy(xall.at[t, s], xall.at[t, s], xm_s.at[s], x_r.at[t, s], ep=mate).start()

    @pl.loop(1, G)
    def _(k):
        g = group(k)
        rcopy(xall.at[t, e], xall.at[t, e], xr_s.at[g], x_r.at[t, e], ep=2 * g + par).start()

    to_mate(e)

    def spread_tp(s):
        rcopy(xall.at[t, s], xall.at[t, s], x2_s.at[s], x_r.at[t, s], tp=across).start()
        rcopy(xall.at[t, s], xall.at[t, s], x1_s.at[0, s], x_r.at[t, s], tp=beside).start()

    def forward(s):
        rcopy(xall.at[across, s], xall.at[across, s], x2_s.at[s], x_r.at[across, s], tp=across).wait_recv()
        rcopy(xall.at[across, s], xall.at[across, s], x1_s.at[1, s], x_r.at[across, s], tp=beside).start()

    def arrived(s, p):
        rcopy(xall.at[t, s], xall.at[t, s], xm_s.at[s], x_r.at[t, s], ep=p).wait_recv()

    spread_tp(e)

    @pl.loop(1, G)
    def _(k):
        s = rail_from(k)
        arrived(s, s)
        to_mate(s)
        spread_tp(s)
        last = mate_of(rail_from(k - 1))
        arrived(last, mate)
        spread_tp(last)
        forward(rail_from(k - 1))

        @pl.when(k > 1)
        def _():
            forward(mate_of(rail_from(k - 2)))

    last = mate_of(rail_from(G - 1))
    arrived(last, mate)
    spread_tp(last)
    forward(rail_from(G - 1))
    if G > 1:
        forward(mate_of(rail_from(G - 2)))
    forward(last)

    @pl.loop(0, E)
    def _(s):
        rcopy(xall.at[beside, s], xall.at[beside, s], x1_s.at[0, s], x_r.at[beside, s], tp=beside).wait_recv()
        rcopy(xall.at[diagonal, s], xall.at[diagonal, s], x1_s.at[1, s], x_r.at[diagonal, s], tp=beside).wait_recv()

    own_dw.wait()
    for j in order:
        rcopy(dwp.at[j], dwr.at[j], dw_s.at[j], dw_r.at[j], tp=j).wait_recv()
    rows = min(N, 512)

    @pl.loop(0, N // rows)
    def _(b):
        hacc[...] = jnp.zeros_like(hacc)
        eb = rows // M

        @pl.loop(0, T)
        def _(q):
            xq = xall[q, pl.ds(b * eb, eb)].reshape(rows, C)
            hacc[...] += dot(xq, dwr[q])

        h = hacc[...]
        half = h.shape[1] // 2
        act = jax.nn.silu(h) * pltpu.roll(h, half, axis=1)
        aall[t, pl.ds(pl.multiple_of(b * rows, 16), rows), :] = act[:, :half].astype(BF16)

    a_across = rcopy(aall.at[t], aall.at[t], a_s.at[0], a_r.at[t], tp=across)
    a_beside = rcopy(aall.at[t], aall.at[t], a_s.at[1], a_r.at[t], tp=beside)
    a_across.start()
    a_beside.start()

    @pl.loop(0, T)
    def _(q):
        cols = pl.ds(pl.multiple_of(q * C, 128), C)
        xe[:, cols] = dot(sel[...], xall[q].reshape(N, C)).astype(BF16)

    loads[1].wait()
    loads[2].wait()
    FH = eg.shape[1]
    nch = 256 if FH % 256 == 0 else FH

    @pl.loop(0, FH // nch)
    def _(n):
        cols = pl.ds(pl.multiple_of(n * nch, 128), nch)
        g = dot(xe[...], eg[:, cols])
        u = dot(xe[...], eu[:, cols])
        hid[:, cols] = (jax.nn.silu(g) * u).astype(BF16)

    a_in = rcopy(aall.at[across], aall.at[across], a_s.at[0], a_r.at[across], tp=across)
    a_in.wait_recv()
    a_fwd = rcopy(aall.at[across], aall.at[across], a_s.at[2], a_r.at[across], tp=beside)
    a_fwd.start()

    loads[3].wait()
    for j in order:
        cols = pl.ds(pl.multiple_of(j * C, 128), C)
        ebuf[j] = dot(hid[...], ed[:, cols]).astype(BF16)
        rcopy(ebuf.at[j], erec.at[t], er_s.at[j], er_r.at[t], tp=j).start()
    ebuf[t] = dot(hid[...], ed[:, own_cols]).astype(BF16)

    loads[4].wait()
    rcopy(aall.at[beside], aall.at[beside], a_s.at[1], a_r.at[beside], tp=beside).wait_recv()
    rcopy(aall.at[diagonal], aall.at[diagonal], a_s.at[2], a_r.at[diagonal], tp=beside).wait_recv()
    red = ebuf[t].astype(F32)
    for j in reversed(order):
        rcopy(ebuf.at[j], erec.at[j], er_s.at[j], er_r.at[j], tp=j).wait_recv()
        red = red + erec[j].astype(F32)
    red = (red.astype(BF16).astype(F32) * w_slot).astype(BF16)
    gate = jax.nn.sigmoid(branch[...])
    ebuf[t] = red
    pair = 2 * M

    def block(g):
        rws = pl.ds(pl.multiple_of(g * pair, 128 if pair % 128 == 0 else 16), pair)
        d = dot(aall[0, rws, :], dd[0])
        for q in range(1, T):
            d = d + dot(aall[q, rws, :], dd[q])
        d = d * gate + lax.dot_general(
            sel[:, rws], ebuf[t], (((0,), (0,)), ((), ())), preferred_element_type=F32
        )
        dtmp[...] = d.reshape(2, M, C)
        om[g] = dtmp[1 - par].astype(BF16)
        rcopy(om.at[g], orm.at[g], om_s.at[g], om_r.at[g], ep=mate).start()
        dacc[g] = dtmp[par]

    def block_on(g):
        rcopy(om.at[g], orm.at[g], om_s.at[g], om_r.at[g], ep=mate).wait_recv()
        oz[g] = (dacc[g] + orm[g].astype(F32)).astype(BF16)
        rcopy(oz.at[g], ozr.at[g0], oz_s.at[g], oz_r.at[g0], ep=2 * g + par).start()

    @pl.loop(1, G)
    def _(k):
        block(group(k))

        @pl.when(k > 1)
        def _():
            block_on(group(k - 1))

    block(g0)
    block_on(group(G - 1))
    rcopy(om.at[g0], orm.at[g0], om_s.at[g0], om_r.at[g0], ep=mate).wait_recv()
    acc[:, :C] = summed_ref[...].astype(F32) + dacc[g0] + orm[g0].astype(F32)

    @pl.loop(1, G)
    def _(k):
        g = group(k)
        rcopy(oz.at[g], ozr.at[g], oz_s.at[g], oz_r.at[g], ep=2 * g + par).wait_recv()
        acc[:, :C] += ozr[g].astype(F32)

    new_hidden[...] = acc[:, :C].astype(BF16)

    @pl.loop(1, E)
    def _(k):
        p = ep_peer(k)
        rcopy(nb.at[p], spread.at[e], nb_s.at[p], nb_r.at[e], ep=p).wait_send()
        rcopy(ct.at[p], ctr.at[e], ct_s.at[p], ct_r.at[e], ep=p).wait_send()

    @pl.loop(0, G)
    def _(g):
        rcopy(pm.at[g], yrec.at[g], pm_s.at[g], pm_r.at[g], ep=mate).wait_send()
        rcopy(om.at[g], orm.at[g], om_s.at[g], om_r.at[g], ep=mate).wait_send()
        s = 2 * g + par
        rcopy(xall.at[t, s], xall.at[t, s], xm_s.at[s], x_r.at[t, s], ep=mate).wait_send()

    @pl.loop(1, G)
    def _(k):
        g = group(k)
        p = 2 * g + par
        rcopy(zout.at[g], zrec.at[g0], pz_s.at[g], pz_r.at[g0], ep=p).wait_send()
        rcopy(oz.at[g], ozr.at[g0], oz_s.at[g], oz_r.at[g0], ep=p).wait_send()
        rcopy(xall.at[t, e], xall.at[t, e], xr_s.at[g], x_r.at[t, e], ep=p).wait_send()

    for j in order:
        rcopy(dwp.at[j], dwr.at[t], dw_s.at[j], dw_r.at[t], tp=j).wait_send()
        rcopy(mbuf.at[j], mrec.at[t], mx_s.at[j], mx_r.at[t], tp=j).wait_send()
        rcopy(qbuf, qrec.at[t], q_s.at[j], q_r.at[t], tp=j).wait_send()
        rcopy(ebuf.at[j], erec.at[t], er_s.at[j], er_r.at[t], tp=j).wait_send()

    @pl.loop(0, E)
    def _(s):
        rcopy(xall.at[t, s], xall.at[t, s], x2_s.at[s], x_r.at[t, s], tp=across).wait_send()
        rcopy(xall.at[t, s], xall.at[t, s], x1_s.at[0, s], x_r.at[t, s], tp=beside).wait_send()
        rcopy(xall.at[across, s], xall.at[across, s], x1_s.at[1, s], x_r.at[across, s], tp=beside).wait_send()

    a_across.wait_send()
    a_beside.wait_send()
    a_fwd.wait_send()


def on_device(
    hidden, mix_gain, proj_x, proj_y, conv_taps, input_gate, decay_gate, decay_param,
    proj_out, conv_state, lru_state, ffn_gain, routes, route_weights,
    expert_gate, expert_up, expert_down, dense_gate, dense_up, dense_down, branch_gate,
):
    E = lax.axis_size("ep")
    T = lax.axis_size("tp")
    M, D = hidden.shape
    C = D // T
    R = proj_x.shape[0]
    N = E * M
    heads, block = input_gate.shape[:2]
    group = max(1, 128 // block)

    experts = expert_gate.shape[0] * E
    capacity = M * routes.shape[1] // experts + 2
    slots = -(-E * capacity // 16) * 16
    G = E // 2
    h = dense_gate.shape[1] // T
    half = -(-2 * h // 128) * 64

    dd = jnp.pad(dense_down.reshape(T, h, C), ((0, 0), (0, half - h), (0, 0)))
    FH = expert_gate.shape[2]
    vm = pl.BlockSpec(memory_space=pltpu.VMEM)
    anyspace = pl.BlockSpec(memory_space=pl.ANY)
    DMA = pltpu.SemaphoreType.DMA
    V = pltpu.VMEM
    rows = min(N, 512)
    scratch = [
        V((E, 1, M), F32), V((1, N), F32), V((heads // group, group * block, 2 * group * block), BF16),
        V((R, C), BF16), V((R, C), BF16), V((C, T * h), BF16), V((C, T * h), BF16),
        V((C, D), BF16), V((D, FH), BF16), V((D, FH), BF16), V((FH, D), BF16), V((T, half, C), BF16),
        V((E, M, R), BF16), V((T, C, 2 * half), BF16), V((T, C, 2 * half), BF16),
        V((E, M, R), BF16), V((G, M, 2 * C), BF16), V((G, M, 2 * C), F32), V((G, M, 2 * C), BF16),
        V((G, M, 2 * C), BF16), V((G, M, 2 * C), BF16), V((E, 1, M), F32), V((M, 2 * C), F32),
        V((T, M, C), BF16), V((T, M, C), BF16), V((M, 128), F32), V((T, M, 128), F32),
        V((T, E, M, C), BF16), V((rows, 2 * half), F32), V((T, N, half), BF16),
        V((slots, D), BF16), V((slots, FH), BF16), V((slots, N), BF16),
        V((T, slots, C), BF16), V((T, slots, C), BF16), V((2, M, C), F32),
        V((G, M, C), BF16), V((G, M, C), F32), V((G, M, C), BF16), V((G, M, C), BF16), V((G, M, C), BF16),
        V((M, C), BF16),
        DMA((10,)),
        DMA((E,)), DMA((E,)), DMA((E,)), DMA((E,)), DMA((G,)), DMA((G,)), DMA((G,)), DMA((G,)),
        DMA((T,)), DMA((T,)), DMA((T,)), DMA((T,)), DMA((T,)), DMA((T,)),
        DMA((G,)), DMA((E,)), DMA((E,)), DMA((2, E)), DMA((T, E)), DMA((3,)), DMA((T,)), DMA((T,)), DMA((T,)),
        DMA((G,)), DMA((G,)), DMA((G,)), DMA((G,)),
    ]
    new_hidden, new_lru, x_new = pl.pallas_call(
        functools.partial(layer_kernel, E, T, slots),
        out_shape=(
            jax.ShapeDtypeStruct((M, C), BF16),
            jax.ShapeDtypeStruct((M, C), F32),
            jax.ShapeDtypeStruct((M, C), BF16),
        ),
        in_specs=[vm] * 12 + [anyspace] * 9,
        out_specs=(vm, vm, vm),
        scratch_shapes=scratch,
        compiler_params=pltpu.CompilerParams(
            collective_id=0, has_side_effects=True, vmem_limit_bytes=60 * 1024 * 1024
        ),
    )(
        hidden, mix_gain[None, :], routes.T, route_weights.T, conv_state.transpose(1, 0, 2), conv_taps,
        input_gate, decay_gate, decay_param[None, :], lru_state,
        ffn_gain[None, :], branch_gate[None, :],
        proj_x, proj_y, dense_gate, dense_up, proj_out, expert_gate[0], expert_up[0], expert_down[0], dd,
    )
    new_conv = jnp.concatenate([conv_state[:, 1:], x_new[:, None, :]], axis=1)
    return (new_hidden, new_lru, new_conv)


def solution(mesh):
    in_specs = (
        P("ep", None),
        P(),
        P("ep", "tp"),
        P("ep", "tp"),
        P(None, "tp"),
        P("tp", None, None),
        P("tp", None, None),
        P("tp"),
        P("tp", None),
        P("ep", None, "tp"),
        P("ep", "tp"),
        P(),
        P("ep", None),
        P("ep", None),
        P("ep", None, "tp"),
        P("ep", None, "tp"),
        P("ep", "tp", None),
        P("tp", "ep"),
        P("tp", "ep"),
        P("ep", "tp"),
        P("tp"),
    )
    out_specs = (P("ep", "tp"), P("ep", "tp"), P("ep", None, "tp"))
    return jax.shard_map(
        on_device, mesh=mesh, in_specs=in_specs, out_specs=out_specs, check_vma=False
    )
```
